256 devices in a mesh: sp: 16 (over y, x), tp: 16 (over z, core).
Axes of the slice: x: 4, y: 4, z: 8, core: 2. Of those that a mesh axis runs over, the one named last changes fastest.
Arguments:
- query_input: bfloat16 [1024, 4096], P('tp', 'sp'), may hold values from -6 to 6
- key_input: bfloat16 [1024, 4096], P('tp', 'sp'), may hold values from -6 to 6
- retrieved_content_matrix: bfloat16 [1024, 4096], P('tp', 'sp'), may hold values from -6 to 6
- gate_input: bfloat16 [1024, 4096], P('tp', 'sp'), may hold values from -6 to 6
- log_decay: float32 [2, 16, 4096], P(None, 'tp', 'sp'), may hold values from -2 to 0
- residual: bfloat16 [4096, 2048], P(('sp', 'tp')), may hold values from -6 to 6
- out_weight: bfloat16 [1024, 2048], replicated, may hold values from -0.1875 to 0.1875
- norm_gain: bfloat16 [2048], replicated, may hold values from 0.099609375 to 1.8984375
- routes: int32 [4096, 2], P(('sp', 'tp')), may hold values from 0 to 15, all different within a row; in each aligned block of 16 rows (0 to 15, 16 to 31, ...) at most 3 rows name the same one
- route_weight: float32 [4096, 2], P(('sp', 'tp')), may hold values from 0.1 to 1
- gate_weight: bfloat16 [16, 2048, 5504], P('sp', None, 'tp'), may hold values from -0.125 to 0.125
- up_weight: bfloat16 [16, 2048, 5504], P('sp', None, 'tp'), may hold values from -0.125 to 0.125
- down_weight: bfloat16 [16, 5504, 2048], P('sp', 'tp'), may hold values from -0.078125 to 0.078125
Outputs:
- output: bfloat16 [4096, 2048], P(('sp', 'tp'))
The draws below stay inside these ranges and needn't reach their ends.
Inputs may be any that keep to these rules, and one draw needn't show every extreme that they name: `routes`: each row names 2 different experts. In each aligned block of 16 rows no expert is named by more than 3 rows, a bound that some block reaches.
All inputs are finite; a program needn't handle non-finite values.
Results may differ from the reference program's by a relative error of at most 0.015.
Values may be sent and summed in bfloat16 or wider, within the bound.
A program may use at most 64 MiB of HBM per device.

```python
import math
import jax
import jax.numpy as jnp
import numpy as np
from jax import lax

D = 2048
HEADS = 16
HEAD_DIM = 64
RET_W = 1024
FF = 5504
FF_DEV = 344
EXPERTS = 16
TOP = 2
TOK_DEV = 256
TOK_TP = 16
TOKENS = 4096
CAP = 3
N_TP = 16


def draw_log_decay(key, part):
    streams = jax.random.split(key, 9)
    blocks = TOKENS // TOK_DEV
    sluggish_tally = HEADS // 2
    order_forward = jax.random.permutation(streams[0], HEADS)
    order_backward = jax.random.permutation(streams[1], HEADS)
    slow = jnp.stack([order_forward < sluggish_tally, order_backward < sluggish_tally])
    slow_rate = jax.random.uniform(streams[2], (2, HEADS), jnp.float32, 0.15, 0.4) / TOKENS
    fast_rate = jax.random.uniform(streams[3], (2, HEADS), jnp.float32, 0.015, 0.03)
    rate = jnp.where(slow, slow_rate, fast_rate)
    parity = jax.random.randint(streams[4], (), 0, 2)
    signs = jnp.where((jnp.arange(blocks) + parity) % 2 == 0, 1.0, -1.0)
    levels = jax.random.uniform(streams[5], (2, 1, blocks), jnp.float32, 0.5, 1.0)
    factor = jnp.repeat(jnp.exp2(signs[None, None, :] * levels), TOK_DEV, axis=2)
    rough = jax.random.uniform(streams[6], (2, HEADS, TOKENS), jnp.float32, 0.5, 1.5)
    starting_displacement = -rate[:, :, None] * factor * rough
    bucket_locations = jax.random.randint(streams[7], (2, HEADS, 2), 0, TOKENS)
    portion_quantities = jax.random.uniform(streams[8], (2, HEADS, 2), jnp.float32, math.log(0.5), math.log(0.8))
    element_locations = jnp.arange(TOKENS)
    element_runs = jnp.sum(jnp.where(element_locations[None, None, None, :] == bucket_locations[..., None], portion_quantities[..., None], 0.0), axis=2)
    return (starting_displacement + element_runs).astype(jnp.float32)


def level_of(key, dims, shards, least, largest):
    loudness, own = 1.0, jax.random.fold_in(key, 6)
    for dim, shards_of in shards:
        steps = jnp.exp(jax.random.uniform(jax.random.fold_in(own, dim), (shards_of,), jnp.float32, least / len(shards), largest / len(shards)))
        loudness = loudness * jnp.repeat(steps, dims[dim] // shards_of).reshape([-1 if axis == dim else 1 for axis in range(len(dims))])
    return loudness


def assign_block(own_key, own, number, rows, number_of, top, most, lean):
    order = jax.random.permutation(own_key, number_of)
    crowded, usual = portions_of(number_of, rows * top, most, lean, True), portions_of(number_of, rows * top, most, lean, False)
    places = jnp.arange(number_of)

    def named(sizes, rotation):
        used = int((sizes > 0).sum())
        fixed = max(1, used // 4)
        shifted = fixed + (places - fixed + rotation * (used - fixed)) % max(1, number_of - fixed)
        return jnp.zeros((number_of,), jnp.int32).at[order[jnp.where(places < fixed, places, shifted)]].set(jnp.asarray(sizes, jnp.int32))

    sizes = jnp.where(number % 4 == 0, named(crowded, number // 4), named(usual, number - number // 4 - 1))
    mixed = jax.random.permutation(jax.random.fold_in(own, 3), number_of)
    giver, receiver = mixed[0:number_of // 2 * 2:2], mixed[1:number_of // 2 * 2:2]
    margin = jnp.minimum(sizes[giver] - 1, most - sizes[receiver]) // 2
    margin = jnp.where((giver == order[0]) | (receiver == order[0]) | (sizes[receiver] == 0), 0, jnp.maximum(margin, 0))
    shifted = jax.random.randint(jax.random.fold_in(own, 4), (number_of // 2,), 0, 1 << 20) % (margin + 1)
    sizes = sizes.at[giver].add(-shifted).at[receiver].add(shifted)
    members = jnp.searchsorted(jnp.cumsum(sizes), jnp.arange(rows * top), side="right").astype(jnp.int32)
    table = members.reshape(top, rows).T
    table = table[jax.random.permutation(jax.random.fold_in(own, 1), rows)]
    rotation = jax.random.randint(jax.random.fold_in(own, 2), (rows, 1), 0, top)
    return jnp.take_along_axis(table, (jnp.arange(top)[None, :] + rotation) % top, axis=1)


def portions_of(count, total, reach, lean, full):
    loads = [(1 << 20) // math.isqrt(standing ** lean) + 1 for standing in range(1, count + 1)]
    largest = reach if full else min(reach, max(-(-total // count), total * loads[0] // sum(loads)))
    least = 1 if total - largest >= count - 1 else 0
    counts, surplus = [largest] + [least] * (count - 1), total - largest - least * (count - 1)
    while surplus > 0:
        candidates = [i for i in range(1, count) if counts[i] < largest] or [i for i in range(1, count) if counts[i] < reach]
        pool, budget = sum([loads[i] for i in candidates]), surplus
        for i in candidates:
            extra = min(reach - counts[i], max(1, budget * loads[i] // pool), surplus)
            counts[i] = counts[i] + extra
            surplus = surplus - extra
    return np.array(counts)


def gaussian(stream_key, extent, spread, limit, shards=(), held_as=jnp.bfloat16):
    result = jax.random.normal(stream_key, extent, jnp.float32) * spread
    if len(shards) > 0:
        result = level_of(stream_key, extent, shards, -0.22, 0.18) * result
    return jnp.clip(result, min=-limit, max=limit).astype(held_as)


def setup_inputs(seed: int = 0) -> dict:
    splits = jax.random.split(jax.random.key(seed), 14)
    query_input = gaussian(splits[0], (RET_W, TOKENS), 1.0, 6.0, ((0, 16), (1, 16)))
    key_input = gaussian(splits[1], (RET_W, TOKENS), 1.0, 6.0, ((0, 16), (1, 16)))
    retrieved_content_matrix = gaussian(splits[2], (RET_W, TOKENS), 1.0, 6.0, ((0, 16), (1, 16)))
    gate_input = gaussian(splits[3], (RET_W, TOKENS), 1.0, 6.0, ((0, 16), (1, 16)))
    log_decay = draw_log_decay(jax.random.fold_in(splits[13], 71), 0)
    residual = gaussian(splits[5], (TOKENS, D), 1.0, 6.0, ((0, 256),))
    out_weight = gaussian(splits[6], (RET_W, D), RET_W ** -0.5, 0.1875)
    norm_gain = jnp.clip(1.0 + 0.18 * jax.random.normal(splits[7], (D,), jnp.float32), 0.099609375, 1.8984375).astype(jnp.bfloat16)
    routes_keys = jax.random.split(jax.random.fold_in(splits[8], 1), TOKENS // TOK_TP)
    routes_turns = jax.random.permutation(jax.random.fold_in(splits[8], 3), TOKENS // TOK_TP)
    routes = jax.vmap(lambda own, number: assign_block(jax.random.fold_in(splits[8], 2), own, number, TOK_TP, EXPERTS, TOP, CAP, 1))(routes_keys, routes_turns).reshape((TOKENS, TOP))
    route_weight = jnp.clip(0.1 + 0.9 * jax.random.uniform(splits[9], (TOKENS, TOP), jnp.float32) ** level_of(splits[9], (TOKENS, TOP), ((0, 256),), -0.2, 0.2), 0.1, 1.0)
    gate_weight = gaussian(splits[10], (EXPERTS, D, FF), D ** -0.5, 0.125, ((0, 16), (2, 16)))
    up_weight = gaussian(splits[11], (EXPERTS, D, FF), D ** -0.5, 0.125, ((0, 16), (2, 16)))
    down_weight = gaussian(splits[12], (EXPERTS, FF, D), FF ** -0.5, 0.078125, ((0, 16), (1, 16)))
    return {"query_input": query_input, "key_input": key_input, "retrieved_content_matrix": retrieved_content_matrix, "gate_input": gate_input, "log_decay": log_decay, "residual": residual, "out_weight": out_weight, "norm_gain": norm_gain, "routes": routes, "route_weight": route_weight, "gate_weight": gate_weight, "up_weight": up_weight, "down_weight": down_weight}


full_precision = lax.Precision.HIGHEST

def head_norm(values, mesh_axis):
    centred = values - lax.optimization_barrier(jnp.mean(values, axis=mesh_axis, keepdims=True))
    return centred * lax.rsqrt(lax.optimization_barrier(jnp.mean(centred * centred, axis=mesh_axis, keepdims=True)) + 1e-06)

def reference(query_input, key_input, retrieved_content_matrix, gate_input, log_decay, residual, out_weight, norm_gain, routes, route_weight, gate_weight, up_weight, down_weight):
    segment_count = TOKENS // TOK_DEV

    def by_segment(array):
        shaped = array.astype(jnp.float32).reshape(HEADS, HEAD_DIM, segment_count, TOK_DEV)
        return jnp.transpose(shaped, (2, 0, 1, 3))
    queries = by_segment(query_input)
    all_keys = by_segment(key_input)
    all_values = by_segment(retrieved_content_matrix)
    gate_values = by_segment(gate_input)
    forward_log = jnp.transpose(log_decay[0].reshape(HEADS, segment_count, TOK_DEV), (1, 0, 2))
    backward_log = jnp.transpose(log_decay[1].reshape(HEADS, segment_count, TOK_DEV), (1, 0, 2))
    forward_prefix = jnp.cumsum(forward_log, axis=-1)
    backward_prefix = jnp.cumsum(backward_log, axis=-1) - backward_log
    forward_total = forward_prefix[..., -1]
    backward_total = lax.optimization_barrier(jnp.sum(backward_log, axis=-1))
    forward_keys = all_keys * jnp.exp(forward_total[..., None] - forward_prefix)[:, :, None, :]
    backward_keys = all_keys * jnp.exp(backward_prefix)[:, :, None, :]
    local_forward = jnp.einsum('nhds,nhes->nhde', forward_keys, all_values, precision=full_precision)
    backward_local = jnp.einsum('nhds,nhes->nhde', backward_keys, all_values, precision=full_precision)

    def carry_step(state, inputs):
        total, local = inputs
        return (jnp.exp(total)[:, None, None] * state + local, state)
    zero_state = jnp.zeros((HEADS, HEAD_DIM, HEAD_DIM), jnp.float32)
    _, forward_in = lax.scan(carry_step, zero_state, (forward_total, local_forward))
    _, backward_in = lax.scan(carry_step, zero_state, (backward_total, backward_local), reverse=True)
    offsets = jnp.arange(TOK_DEV)
    lower = offsets[:, None] >= offsets[None, :]
    upper = offsets[:, None] <= offsets[None, :]

    def segment_output(inputs):
        query_part, key_part, value_part, forward_part, backward_part, backward_sum, state_fwd, state_bwd = inputs
        scores = jnp.einsum('hdt,hds->hts', query_part, key_part)
        forward_decay_weight = jnp.exp(jnp.where(lower, forward_part[:, :, None] - forward_part[:, None, :], -jnp.inf))
        backward_weight = jnp.exp(jnp.where(upper, backward_part[:, None, :] - backward_part[:, :, None], -jnp.inf))
        weighted = (scores * (forward_decay_weight + backward_weight)).astype(jnp.bfloat16)
        weighted = lax.optimization_barrier(weighted).astype(jnp.float32)
        inner = jnp.einsum('hts,hes->het', weighted, value_part)
        carried = jnp.einsum('hdt,hde->het', query_part, state_fwd, precision=full_precision) * jnp.exp(forward_part)[:, None, :]
        carried = carried + jnp.einsum('hdt,hde->het', query_part, state_bwd, precision=full_precision) * jnp.exp(backward_sum[:, None] - backward_part)[:, None, :]
        return inner + carried
    retained = lax.map(segment_output, (queries, all_keys, all_values, forward_prefix, backward_prefix, backward_total, forward_in, backward_in))
    mixer_out = (head_norm(retained, 2) * jax.nn.silu(gate_values)).astype(jnp.bfloat16)
    mixer_tokens = jnp.transpose(mixer_out, (0, 3, 1, 2)).reshape(TOKENS, RET_W)
    stream = residual.astype(jnp.float32) + jnp.dot(mixer_tokens, out_weight, preferred_element_type=jnp.float32)
    scale = lax.rsqrt(lax.optimization_barrier(jnp.mean(stream * stream, axis=-1, keepdims=True)) + 1e-06)
    normed = (stream * scale * norm_gain.astype(jnp.float32)).astype(jnp.bfloat16)
    slots_total = CAP * (TOKENS // TOK_TP)

    def expert_step(expert, moe_sum):
        chosen = jnp.any(routes == expert, axis=-1)
        picked = jnp.nonzero(chosen, size=slots_total, fill_value=0)[0].astype(jnp.int32)
        valid = (jnp.arange(slots_total) < jnp.sum(chosen.astype(jnp.int32))).astype(jnp.float32)
        inputs = normed[picked]
        gates = jnp.dot(inputs, gate_weight[expert], preferred_element_type=jnp.float32)
        ups = jnp.dot(inputs, up_weight[expert], preferred_element_type=jnp.float32)
        hidden = (jax.nn.silu(gates) * ups).astype(jnp.bfloat16)
        grouped = hidden.reshape(slots_total, N_TP, FF_DEV).astype(jnp.float32)
        down_groups = down_weight[expert].reshape(N_TP, FF_DEV, D).astype(jnp.float32)
        parts = jnp.einsum('rjf,jfd->rjd', grouped, down_groups).astype(jnp.bfloat16)
        parts = lax.optimization_barrier(parts).astype(jnp.float32)
        expert_out = lax.optimization_barrier(jnp.sum(parts, axis=1)).astype(jnp.bfloat16)
        weight = lax.optimization_barrier(jnp.sum(jnp.where(routes[picked] == expert, route_weight[picked], 0.0), axis=-1)) * valid
        return moe_sum.at[picked].add(weight[:, None] * expert_out.astype(jnp.float32))
    moe_sum = lax.fori_loop(0, EXPERTS, expert_step, jnp.zeros((TOKENS, D), jnp.float32))
    return (stream + moe_sum).astype(jnp.bfloat16)
```

```python
import functools

import jax
import jax.numpy as jnp
from jax import lax
from jax.experimental import pallas as pl
from jax.experimental.pallas import tpu as pltpu
from jax.sharding import PartitionSpec as P

HD = 64
D = 2048
FFD = 344
SP = 16
TPN = 16
NZ = 8
SEG = 256
TOK = 16
CAP = 3
ROWS = SP * CAP
HALF = D // 2
LANES = 128
NCH = D // LANES
F32 = jnp.float32
BF16 = jnp.bfloat16
MESH = pl.DeviceIdType.MESH


def contract(a, b, da, db):
    return lax.dot_general(a, b, (((da,), (db,)), ((), ())), preferred_element_type=F32)


def iota(shape, dim):
    return lax.broadcasted_iota(jnp.int32, shape, dim)


def kernel(
    q_ref,
    k_ref,
    v_ref,
    g_ref,
    ld_ref,
    res_ref,
    gain_ref,
    routes_ref,
    rw_ref,
    w_any,
    wg_any,
    wu_any,
    wd_any,
    out_ref,
    w_ref,
    wg_ref,
    wu_ref,
    wd_ref,
    st_ref,
    ysend_ref,
    yrecv_ref,
    stream_ref,
    tmp_ref,
    rsend_ref,
    rrecv_ref,
    ag_ref,
    part_ref,
    sib_ref,
    rs_send_ref,
    rs_recv_ref,
    bsend_ref,
    brecv_ref,
    wsem,
    st_ssem,
    st_rsem,
    y_ssem,
    y_rsem,
    r_ssem,
    r_rsem,
    ag_ssem,
    ag_rsem,
    mir_ssem,
    mir_rsem,
    sib_ssem,
    sib_rsem,
    rs_ssem,
    rs_rsem,
    b_ssem,
    b_rsem,
):
    me_s = lax.axis_index("sp")
    me_t = lax.axis_index("tp")
    z = me_t // 2
    core = me_t % 2
    other = 1 - core
    z_up = ((z + 1) % NZ) * 2 + core
    z_dn = ((z + NZ - 1) % NZ) * 2 + core
    sibling = z * 2 + other

    def remote(src, dst, ssem, rsem, where):
        return pltpu.make_async_remote_copy(
            src_ref=src, dst_ref=dst, send_sem=ssem, recv_sem=rsem, device_id=where, device_id_type=MESH
        )

    barrier = pltpu.get_barrier_semaphore()

    @pl.loop(1, SP)
    def _(j):
        pl.semaphore_signal(barrier, inc=1, device_id={"sp": (me_s + j) % SP}, device_id_type=MESH)
        pl.semaphore_signal(barrier, inc=1, device_id={"tp": (me_t + j) % TPN}, device_id_type=MESH)

    weights = [
        pltpu.make_async_copy(w_any, w_ref, wsem.at[0]),
        pltpu.make_async_copy(wg_any.at[0], wg_ref, wsem.at[1]),
        pltpu.make_async_copy(wu_any.at[0], wu_ref, wsem.at[2]),
        pltpu.make_async_copy(wd_any.at[0], wd_ref, wsem.at[3]),
    ]
    for copy in weights:
        copy.start()

    lf = ld_ref[0]
    lb = ld_ref[1]
    at_t = iota((SEG, SEG), 0)
    at_s = iota((SEG, SEG), 1)
    cf_col = jnp.sum(jnp.where(at_s <= at_t, lf, 0.0), axis=1, keepdims=True)
    eb_col = jnp.sum(jnp.where(at_s < at_t, lb, 0.0), axis=1, keepdims=True)
    cf = jnp.sum(jnp.where(at_s == at_t, cf_col, 0.0), axis=0, keepdims=True)
    eb = jnp.sum(jnp.where(at_s == at_t, eb_col, 0.0), axis=0, keepdims=True)
    total_f = jnp.sum(lf, axis=1, keepdims=True)
    total_b = jnp.sum(lb, axis=1, keepdims=True)
    q = q_ref[...]
    keys = k_ref[...]
    vals = v_ref[...]
    wide_keys = keys.astype(F32)
    kf = (wide_keys * jnp.exp(jnp.minimum(total_f - cf, 0.0))).astype(BF16)
    kb = (wide_keys * jnp.exp(eb)).astype(BF16)
    f_loc = contract(kf, vals, 1, 1)
    g_loc = contract(kb, vals, 1, 1)
    lane = iota((1, LANES), 1)
    totals = jnp.where(lane < HD, total_f, total_b)
    hi = totals.astype(BF16).astype(F32)
    mid = (totals - hi).astype(BF16).astype(F32)
    low = totals - hi - mid
    row16 = iota((16, LANES), 0)
    packed = jnp.where(row16 == 0, hi, jnp.where(row16 == 1, mid, jnp.where(row16 == 2, low, 0.0)))
    st_ref[me_s, pl.ds(0, HD), :] = jnp.concatenate([f_loc, g_loc], axis=1).astype(BF16)
    st_ref[me_s, pl.ds(HD, 16), :] = packed.astype(BF16)

    pl.semaphore_wait(barrier, 2 * (SP - 1))

    def st_copy(j):
        p = (me_s + j) % SP
        return remote(st_ref.at[me_s], st_ref.at[me_s], st_ssem.at[p], st_rsem.at[me_s], {"sp": p})

    @pl.loop(1, SP)
    def _(j):
        st_copy(j).start()

    scores = contract(q, keys, 0, 0)
    w = jnp.where(at_s <= at_t, jnp.exp(jnp.minimum(cf_col - cf, 0.0)), 0.0)
    w = w + jnp.where(at_s >= at_t, jnp.exp(jnp.minimum(eb - eb_col, 0.0)), 0.0)
    p_mat = (scores * w).astype(BF16)
    inner = contract(vals, p_mat, 1, 1)
    gates = g_ref[...].astype(F32)
    gate_act = gates * jax.nn.sigmoid(gates)

    def st_arrived(j):
        p = (me_s + j) % SP
        return remote(st_ref.at[p], st_ref.at[p], st_ssem.at[p], st_rsem.at[p], {"sp": p})

    @pl.loop(1, SP)
    def _(j):
        st_arrived(j).wait_recv()

    half_lane = iota((HD, LANES), 1) < HD

    def scan(i, acc):
        m_b = SP - 1 - i
        loc = jnp.where(half_lane, st_ref[i, pl.ds(0, HD), :].astype(F32), st_ref[m_b, pl.ds(0, HD), :].astype(F32))
        tail_f = jnp.sum(st_ref[i, pl.ds(HD, 16), :].astype(F32), axis=0, keepdims=True)
        tail_b = jnp.sum(st_ref[m_b, pl.ds(HD, 16), :].astype(F32), axis=0, keepdims=True)
        decay = jnp.exp(jnp.where(lane < HD, tail_f, tail_b))
        step_f = (i < me_s).astype(jnp.int32)
        step_b = (m_b > me_s).astype(jnp.int32)
        use = jnp.where(half_lane, step_f, step_b) > 0
        return jnp.where(use, decay * acc + loc, acc)

    state = lax.fori_loop(0, SP, scan, jnp.zeros((HD, LANES), F32))
    state_hi = state.astype(BF16)
    state_lo = (state - state_hi.astype(F32)).astype(BF16)
    carried = contract(state_hi, q, 0, 0) + contract(state_lo, q, 0, 0)
    o = inner + carried[:HD] * jnp.exp(cf) + carried[HD:] * jnp.exp(jnp.minimum(total_b - eb, 0.0))
    o = o - jnp.mean(o, axis=0, keepdims=True)
    o = o * lax.rsqrt(jnp.mean(o * o, axis=0, keepdims=True) + 1e-06)
    y = o * gate_act
    odd = core.astype(F32)
    both = jnp.concatenate([y * (1.0 - odd), y * odd], axis=0)
    ysend_ref[...] = jnp.transpose(both).astype(BF16).reshape(TPN, TOK, LANES)
    yrecv_ref[me_t] = ysend_ref[me_t]

    def y_copy(j):
        p = (me_t + j) % TPN
        return remote(ysend_ref.at[p], yrecv_ref.at[me_t], y_ssem.at[p], y_rsem.at[me_t], {"tp": p})

    @pl.loop(1, TPN)
    def _(j):
        y_copy(j).start()

    row_e = iota((ROWS, TOK), 0) // CAP
    row_r = iota((ROWS, TOK), 0) % CAP
    first = routes_ref[pl.ds(0, 1), :] == row_e
    named = jnp.logical_or(first, routes_ref[pl.ds(1, 1), :] == row_e)
    earlier = (iota((TOK, TOK), 0) < iota((TOK, TOK), 1)).astype(F32).astype(BF16)
    rank = jnp.dot(named.astype(F32).astype(BF16), earlier, preferred_element_type=F32)
    placed = jnp.logical_and(named, rank == row_r.astype(F32))
    placing = placed.astype(F32).astype(BF16)
    share = jnp.where(placed, jnp.where(first, rw_ref[pl.ds(0, 1), :], rw_ref[pl.ds(1, 1), :]), 0.0)
    share_hi = share.astype(BF16)
    share_lo = (share - share_hi.astype(F32)).astype(BF16)

    weights[0].wait()

    def y_arrived(j):
        p = (me_t + j) % TPN
        return remote(ysend_ref.at[p], yrecv_ref.at[p], y_ssem.at[p], y_rsem.at[p], {"tp": p})

    @pl.loop(1, TPN)
    def _(j):
        y_arrived(j).wait_recv()

    y_tok = jnp.concatenate([yrecv_ref[2 * i] + yrecv_ref[2 * i + 1] for i in range(NZ)], axis=1)
    square = jnp.zeros((TOK, 1), F32)
    for n in range(4):
        cols = pl.ds(n * 512, 512)
        part = res_ref[:, cols].astype(F32) + jnp.dot(y_tok, w_ref[:, cols], preferred_element_type=F32)
        stream_ref[:, cols] = part
        square = square + jnp.sum(part * part, axis=1, keepdims=True)
    scale = lax.rsqrt(square * (1.0 / D) + 1e-06)
    gain = gain_ref[...].astype(F32)
    for c in range(NCH):
        cols = pl.ds(c * LANES, LANES)
        normed = (stream_ref[:, cols] * scale * gain[c : c + 1, :]).astype(BF16)
        tmp_ref[:, c, :] = jnp.dot(placing, normed, preferred_element_type=F32)
    rsend_ref[...] = tmp_ref[...].astype(BF16)
    rrecv_ref[pl.ds(me_s * CAP, CAP)] = rsend_ref[pl.ds(me_s * CAP, CAP)]

    def r_copy(j):
        p = (me_s + j) % SP
        return remote(
            rsend_ref.at[pl.ds(p * CAP, CAP)], rrecv_ref.at[pl.ds(me_s * CAP, CAP)], r_ssem.at[p], r_rsem.at[me_s], {"sp": p}
        )

    @pl.loop(1, SP)
    def _(j):
        r_copy(j).start()

    def r_arrived(j):
        p = (me_s + j) % SP
        return remote(
            rsend_ref.at[pl.ds(p * CAP, CAP)], rrecv_ref.at[pl.ds(p * CAP, CAP)], r_ssem.at[p], r_rsem.at[p], {"sp": p}
        )

    @pl.loop(1, SP)
    def _(j):
        r_arrived(j).wait_recv()

    tmp_ref[...] = rrecv_ref[...].astype(F32)
    for c in range(NCH):
        ag_ref[0, core, :, pl.ds(c * LANES, LANES)] = tmp_ref[:, c, :].astype(BF16)

    def slot(d, k):
        return 0 if k == 0 else (7 if k == 4 else 2 * k - 1 + d)

    def hops(d, h):
        return 4 if d == h else 3

    def ag_send(d, h, k):
        cols = pl.ds(h * HALF, HALF)
        return remote(
            ag_ref.at[slot(d, k), core, :, cols],
            ag_ref.at[slot(d, k + 1), core, :, cols],
            ag_ssem.at[d, h, k],
            ag_rsem.at[d, h, k],
            {"tp": z_up if d == 0 else z_dn},
        )

    def mirror(d, h, k):
        cols = pl.ds(h * HALF, HALF)
        view = ag_ref.at[slot(d, k), core, :, cols]
        return remote(view, view, mir_ssem.at[d, h, k], mir_rsem.at[d, h, k], {"tp": sibling})

    def mirrored(d, h, k):
        cols = pl.ds(h * HALF, HALF)
        view = ag_ref.at[slot(d, k), other, :, cols]
        return remote(view, view, mir_ssem.at[d, h, k], mir_rsem.at[d, h, k], {"tp": sibling})

    def experts(s0, n):
        x = ag_ref[pl.ds(s0, n)].reshape(n * 2 * ROWS, D)
        a = contract(x, wg_ref[...], 1, 1)
        b = contract(x, wu_ref[...], 1, 1)
        hidden = (a * jax.nn.sigmoid(a) * b).astype(BF16)
        part_ref[pl.ds(s0, n)] = (
            jnp.dot(hidden, wd_ref[...], preferred_element_type=F32).astype(BF16).reshape(n, 2, ROWS, D)
        )

    def pair(s):
        return remote(part_ref.at[s, other], sib_ref.at[s], sib_ssem.at[s], sib_rsem.at[s], {"tp": sibling})

    for h in (0, 1):
        for d in (0, 1):
            ag_send(d, h, 0).start()
    for h in (0, 1):
        mirror(0, h, 0).start()
    for copy in weights[1:]:
        copy.wait()
    for h in (0, 1):
        mirrored(0, h, 0).wait_recv()
    experts(0, 1)
    pair(0).start()
    for k in range(1, 5):
        units = [(d, h) for (d, h) in ((0, 0), (1, 1), (0, 1), (1, 0)) if hops(d, h) >= k]
        for d, h in units:
            ag_send(d, h, k - 1).wait_recv()
            if hops(d, h) > k:
                ag_send(d, h, k).start()
            mirror(d, h, k).start()
        for d, h in units:
            mirrored(d, h, k).wait_recv()
        if k < 4:
            experts(2 * k - 1, 2)
            pair(2 * k - 1).start()
            pair(2 * k).start()
        else:
            experts(7, 1)
            pair(7).start()

    def rs_send(d, h, k):
        return remote(
            rs_send_ref.at[d, h, k - 1],
            rs_recv_ref.at[d, h, k - 1],
            rs_ssem.at[d, h, k - 1],
            rs_rsem.at[d, h, k - 1],
            {"tp": z_dn if d == 0 else z_up},
        )

    def pair_sum(s, h):
        cols = pl.ds(h * HALF, HALF)
        return part_ref[s, core, :, cols].astype(F32) + sib_ref[s, :, cols].astype(F32)

    def pair_arrived(s):
        pair(s).wait_recv()

    for s in range(8):
        pair_arrived(s)
    for k in range(4, 0, -1):
        fresh = [(d, h) for d in (0, 1) for h in (0, 1) if hops(d, h) == k]
        later = [(d, h) for d in (0, 1) for h in (0, 1) if hops(d, h) > k]
        if k < 3:
            later = [(0, 1), (1, 0), (0, 0), (1, 1)]
        for d, h in fresh + later:
            acc = pair_sum(slot(d, k), h)
            if (d, h) in later:
                rs_send(d, h, k + 1).wait_recv()
                acc = acc + rs_recv_ref[d, h, k].astype(F32)
            rs_send_ref[d, h, k - 1] = acc.astype(BF16)
            rs_send(d, h, k).start()
    for h in (0, 1):
        acc = pair_sum(0, h)
        for d in (0, 1):
            rs_send(d, h, 1).wait_recv()
            acc = acc + rs_recv_ref[d, h, 0].astype(F32)
        for c in range(NCH // 2):
            tmp_ref[:, h * (NCH // 2) + c, :] = acc[:, c * LANES : (c + 1) * LANES]
    bsend_ref[...] = tmp_ref[...].astype(BF16)
    brecv_ref[pl.ds(me_s * CAP, CAP)] = bsend_ref[pl.ds(me_s * CAP, CAP)]

    def b_copy(j):
        p = (me_s + j) % SP
        return remote(
            bsend_ref.at[pl.ds(p * CAP, CAP)], brecv_ref.at[pl.ds(me_s * CAP, CAP)], b_ssem.at[p], b_rsem.at[me_s], {"sp": p}
        )

    def b_arrived(j):
        p = (me_s + j) % SP
        return remote(
            bsend_ref.at[pl.ds(p * CAP, CAP)], brecv_ref.at[pl.ds(p * CAP, CAP)], b_ssem.at[p], b_rsem.at[p], {"sp": p}
        )

    @pl.loop(1, SP)
    def _(j):
        b_copy(j).start()

    @pl.loop(1, SP)
    def _(j):
        st_copy(j).wait_send()
        y_copy(j).wait_send()
        r_copy(j).wait_send()

    for d in (0, 1):
        for h in (0, 1):
            for k in range(hops(d, h)):
                ag_send(d, h, k).wait_send()
                rs_send(d, h, k + 1).wait_send()
                mirror(d, h, k + 1).wait_send()
    for h in (0, 1):
        mirror(0, h, 0).wait_send()
    for s in range(8):
        pair(s).wait_send()

    @pl.loop(1, SP)
    def _(j):
        b_arrived(j).wait_recv()

    tmp_ref[...] = brecv_ref[...].astype(F32)
    for c in range(NCH):
        cols = pl.ds(c * LANES, LANES)
        back = tmp_ref[:, c, :].astype(BF16)
        moe = contract(share_hi, back, 0, 0) + contract(share_lo, back, 0, 0)
        out_ref[:, cols] = (stream_ref[:, cols] + moe).astype(BF16)

    @pl.loop(1, SP)
    def _(j):
        b_copy(j).wait_send()


def on_device(q, k, v, g, ld, res, w, gain, routes, rw, wg, wu, wd):
    vmem = pl.BlockSpec(memory_space=pltpu.VMEM)
    hbm = pl.BlockSpec(memory_space=pl.ANY)
    dma = pltpu.SemaphoreType.DMA
    return pl.pallas_call(
        kernel,
        out_shape=jax.ShapeDtypeStruct((TOK, D), BF16),
        in_specs=[vmem] * 9 + [hbm] * 4,
        out_specs=vmem,
        scratch_shapes=[
            pltpu.VMEM((1024, D), BF16),
            pltpu.VMEM((FFD, D), BF16),
            pltpu.VMEM((FFD, D), BF16),
            pltpu.VMEM((FFD, D), BF16),
            pltpu.VMEM((SP, HD + 16, LANES), BF16),
            pltpu.VMEM((TPN, TOK, LANES), BF16),
            pltpu.VMEM((TPN, TOK, LANES), BF16),
            pltpu.VMEM((TOK, D), F32),
            pltpu.VMEM((ROWS, NCH, LANES), F32),
            pltpu.VMEM((ROWS, NCH, LANES), BF16),
            pltpu.VMEM((ROWS, NCH, LANES), BF16),
            pltpu.VMEM((8, 2, ROWS, D), BF16),
            pltpu.VMEM((8, 2, ROWS, D), BF16),
            pltpu.VMEM((8, ROWS, D), BF16),
            pltpu.VMEM((2, 2, 4, ROWS, HALF), BF16),
            pltpu.VMEM((2, 2, 4, ROWS, HALF), BF16),
            pltpu.VMEM((ROWS, NCH, LANES), BF16),
            pltpu.VMEM((ROWS, NCH, LANES), BF16),
            dma((4,)),
            dma((SP,)),
            dma((SP,)),
            dma((TPN,)),
            dma((TPN,)),
            dma((SP,)),
            dma((SP,)),
            dma((2, 2, 4)),
            dma((2, 2, 4)),
            dma((2, 2, 5)),
            dma((2, 2, 5)),
            dma((8,)),
            dma((8,)),
            dma((2, 2, 4)),
            dma((2, 2, 4)),
            dma((SP,)),
            dma((SP,)),
        ],
        compiler_params=pltpu.CompilerParams(
            collective_id=0, has_side_effects=True, vmem_limit_bytes=60 * 1024 * 1024
        ),
    )(
        q,
        k,
        v,
        g,
        ld,
        res,
        gain.reshape(NCH, LANES),
        routes.T,
        rw.T,
        w,
        jnp.swapaxes(wg, 1, 2),
        jnp.swapaxes(wu, 1, 2),
        wd,
    )


def solution(mesh):
    return jax.shard_map(
        on_device,
        mesh=mesh,
        in_specs=(
            P("tp", "sp"),
            P("tp", "sp"),
            P("tp", "sp"),
            P("tp", "sp"),
            P(None, "tp", "sp"),
            P(("sp", "tp"), None),
            P(),
            P(),
            P(("sp", "tp"), None),
            P(("sp", "tp"), None),
            P("sp", None, "tp"),
            P("sp", None, "tp"),
            P("sp", "tp", None),
        ),
        out_specs=P(("sp", "tp"), None),
        check_vma=False,
    )
```
